32 devices in a mesh: ra: 4 (over z), cb: 8 (over y, x, core).
Axes of the slice: x: 2, y: 2, z: 4, core: 2. Of those that a mesh axis runs over, the one named last changes fastest.
Arguments:
- tokens: bfloat16 [512, 3072], P(None, 'ra'), may hold values from -14 to 14, as said below
- norm_gain: float32 [2, 3072], P(None, 'ra'), may hold values from 0.1 to 1.9
- gate_weight: float32 [2, 3072, 8448], P(None, 'ra', 'cb'), may hold values from -0.109375 to 0.109375
- gate_scale: float32 [2, 8448], P(None, 'cb'), may hold values from 0.5 to 2
- value_weight: float32 [2, 3072, 8448], P(None, 'ra', 'cb'), may hold values from -0.109375 to 0.109375
- value_scale: float32 [2, 8448], P(None, 'cb'), may hold values from 0.5 to 2
- gate_conv: float32 [2, 3, 8448], P(None, None, 'cb'), may hold values from -3.5 to 3.5
- value_conv: float32 [2, 3, 8448], P(None, None, 'cb'), may hold values from -3.5 to 3.5
- gate_bias: float32 [2, 8448], P(None, 'cb'), may hold values from -3 to 3
- value_bias: float32 [2, 8448], P(None, 'cb'), may hold values from -3 to 3
- down_weight: float32 [2, 8448, 3072], P(None, 'cb', 'ra'), may hold values from -0.0625 to 0.0625
- down_scale: float32 [2, 3072], P(None, 'ra'), may hold values from 0.5 to 2
Outputs:
- stream_out: bfloat16 [512, 3072], P(None, 'ra')
The draws below stay inside these ranges and needn't reach their ends.
Inputs may be any that keep to these rules, and one draw needn't show every extreme that they name: `tokens`: real values; within each token, the blocks of D // 16 consecutive features have scales that differ.
All inputs are finite; a program needn't handle non-finite values.
Results may differ from the reference program's by a relative error of at most 0.039.
Values may be sent and summed in bfloat16 or wider, within the bound.
A program may use at most 64 MiB of HBM per device.

```python
import math
import jax
import jax.numpy as jnp
from jax import lax

D = 3072
FF = 8448
TAPS = 3
LAYERS = 2
SEQ_LEN = 8
TOKENS = 512
N_CB = 8


def draw_tokens(key, part):
    first, second, third = jax.random.split(key, 3)
    scales = jnp.exp(jax.random.uniform(second, (TOKENS, 16), jnp.float32, -1.2, 1.2))
    widths = jnp.repeat(scales, D // 16, axis=1)
    base = jnp.clip(jax.random.normal(first, (TOKENS, D), jnp.float32), -4.0, 4.0)
    return (base * widths).astype(jnp.bfloat16)


def levels(own_key, dims, shards, smallest, top_value):
    loudness = 1.0
    for position, parts in shards:
        draws = jax.random.uniform(jax.random.fold_in(jax.random.fold_in(own_key, 6), position), (parts,), jnp.float32, smallest / len(shards), top_value / len(shards))
        loudness = loudness * jnp.repeat(jnp.exp(draws), dims[position] // parts).reshape((-1,) + (1,) * (len(dims) - 1 - position))
    return loudness


def centred(own_key, shape, scale, bound, cuts=(), kind=jnp.bfloat16):
    result = scale * jax.random.normal(own_key, shape, jnp.float32)
    if cuts:
        result = result * levels(own_key, shape, cuts, -0.22, 0.18)
    return jnp.clip(result, -bound, bound).astype(kind)


def setup_inputs(seed: int = 0) -> dict:
    arg_keys = jax.random.split(jax.random.key(seed), 13)
    tokens = draw_tokens(jax.random.fold_in(arg_keys[12], 71), 0)
    norm_gain = jnp.clip(1.0 + 0.18 * jax.random.normal(arg_keys[1], (LAYERS, D), jnp.float32), 0.1, 1.9)
    gate_weight = centred(arg_keys[2], (LAYERS, D, FF), D ** -0.5, 0.109375, ((1, 4), (2, 8)), jnp.float32)
    gate_scale = jnp.clip(jnp.exp(math.log(2.0) - 1.3862944 * jax.random.uniform(arg_keys[3], (LAYERS, FF), jnp.float32) ** levels(arg_keys[3], (LAYERS, FF), ((1, 8),), -0.2, 0.2)), 0.5, 2.0)
    value_weight = centred(arg_keys[4], (LAYERS, D, FF), D ** -0.5, 0.109375, ((1, 4), (2, 8)), jnp.float32)
    value_scale = jnp.clip(jnp.exp(math.log(2.0) - 1.3862944 * jax.random.uniform(arg_keys[5], (LAYERS, FF), jnp.float32) ** levels(arg_keys[5], (LAYERS, FF), ((1, 8),), -0.2, 0.2)), 0.5, 2.0)
    gate_conv = centred(arg_keys[6], (LAYERS, TAPS, FF), TAPS ** -0.5, 3.5, ((2, 8),), jnp.float32)
    value_conv = centred(arg_keys[7], (LAYERS, TAPS, FF), TAPS ** -0.5, 3.5, ((2, 8),), jnp.float32)
    gate_bias = centred(arg_keys[8], (LAYERS, FF), 0.5, 3.0, ((1, 8),), jnp.float32)
    value_bias = centred(arg_keys[9], (LAYERS, FF), 0.5, 3.0, ((1, 8),), jnp.float32)
    down_weight = centred(arg_keys[10], (LAYERS, FF, D), FF ** -0.5, 0.0625, ((1, 8), (2, 4)), jnp.float32)
    down_scale = jnp.clip(jnp.exp(math.log(2.0) - 1.3862944 * jax.random.uniform(arg_keys[11], (LAYERS, D), jnp.float32) ** levels(arg_keys[11], (LAYERS, D), ((1, 4),), -0.2, 0.2)), 0.5, 2.0)
    return {"tokens": tokens, "norm_gain": norm_gain, "gate_weight": gate_weight, "gate_scale": gate_scale, "value_weight": value_weight, "value_scale": value_scale, "gate_conv": gate_conv, "value_conv": value_conv, "gate_bias": gate_bias, "value_bias": value_bias, "down_weight": down_weight, "down_scale": down_scale}


epsilon = 1e-06
residual_keep = 0.5

def causal_conv(values, conv_taps, conv_bias):
    row_count, col_count = values.shape
    blocks = values.reshape(row_count // SEQ_LEN, SEQ_LEN, col_count)
    padded = jnp.pad(blocks, ((0, 0), (TAPS - 1, 0), (0, 0)))
    summed = conv_bias + jnp.zeros_like(blocks)
    for offset in range(TAPS):
        summed = summed + padded[:, offset:offset + SEQ_LEN] * conv_taps[offset]
    return summed.reshape(row_count, col_count)

def reference(tokens, norm_gain, gate_weight, gate_scale, value_weight, value_scale, gate_conv, value_conv, gate_bias, value_bias, down_weight, down_scale):
    stream = tokens
    for depth_index in range(LAYERS):
        widened = stream.astype(jnp.float32)
        squares = lax.optimization_barrier(jnp.sum(widened * widened, axis=1, keepdims=True))
        inverse_rms = lax.rsqrt(squares / D + epsilon)
        normed = (widened * norm_gain[depth_index]).astype(jnp.bfloat16)
        gate_pre = jnp.dot(normed, gate_weight[depth_index].astype(jnp.bfloat16), preferred_element_type=jnp.float32) * inverse_rms * gate_scale[depth_index]
        value_pre = jnp.dot(normed, value_weight[depth_index].astype(jnp.bfloat16), preferred_element_type=jnp.float32) * inverse_rms * value_scale[depth_index]
        gate_mixed = causal_conv(gate_pre, gate_conv[depth_index], gate_bias[depth_index])
        value_mixed = causal_conv(value_pre, value_conv[depth_index], value_bias[depth_index])
        hidden = (jax.nn.silu(gate_mixed) * value_mixed).astype(jnp.bfloat16)
        hidden = lax.optimization_barrier(hidden)
        pieces = hidden.astype(jnp.float32).reshape(TOKENS, N_CB, FF // N_CB)
        down_half = lax.optimization_barrier(down_weight[depth_index].astype(jnp.bfloat16))
        down_pieces = down_half.astype(jnp.float32).reshape(N_CB, FF // N_CB, D)
        partial_value = jnp.einsum('tcf,cfd->ctd', pieces, down_pieces)
        rounded = lax.optimization_barrier(partial_value.astype(jnp.bfloat16)).astype(jnp.float32)
        branch = lax.optimization_barrier(jnp.sum(rounded, axis=0)) * down_scale[depth_index]
        stream = (residual_keep * widened + branch).astype(jnp.bfloat16)
    return stream
```

```python
import functools
import jax
import jax.numpy as jnp
from jax import lax
from jax.experimental import pallas as pl
from jax.experimental.pallas import tpu as pltpu
from jax.sharding import PartitionSpec as P

SEQ_LEN = 8
EPSILON = 1e-06
RESIDUAL_KEEP = 0.5
MESH = pl.DeviceIdType.MESH
LANES = 128
FIRST = 1
HOP = 2
BACK = 2
SUM_GAP = 2
GATHER_GAP = 2


def kernel(
    cfg,
    tokens_ref,
    gain_ref,
    gw_ref,
    gs_ref,
    vw_ref,
    vs_ref,
    gc_ref,
    vc_ref,
    gb_ref,
    vb_ref,
    dw_ref,
    ds_ref,
    out_ref,
    stage_g,
    stage_v,
    stage_d,
    wc,
    wd,
    par,
    xs,
    own,
    pin,
    pout,
    hid,
    ro,
    ri,
    w_sem,
    ps,
    pr,
    hs,
    hr,
    rs_s,
    rs_r,
    ag_s,
    ag_r,
):
    R, N, L, n, m, D, F = cfg
    Dl = tokens_ref.shape[1]
    rows = 2 * m
    RG = rows // SEQ_LEN
    CG = N // RG
    Dc = Dl // CG
    taps = gc_ref.shape[0]
    full = F // LANES * LANES
    rest = F - full
    wide = full + LANES
    sq_lane = 2 * rest
    at_last = FIRST + (R - 1) * HOP
    at_down = at_last + (R - 1) * BACK
    at_sum = at_down + SUM_GAP
    at_gather = at_sum + GATHER_GAP
    S = max(n, at_gather)
    z = lax.axis_index("ra")
    me = lax.axis_index("cb")

    def weight_copy(l, k):
        src, dst = ((gw_ref, stage_g), (vw_ref, stage_v), (dw_ref, stage_d))[k]
        return pltpu.make_async_copy(src.at[l], dst, w_sem.at[k])

    for k in range(3):
        weight_copy(0, k).start()

    barrier = pltpu.get_barrier_semaphore()
    for k in range(1, N):
        pl.semaphore_signal(
            barrier, inc=1, device_id={"cb": lax.rem(me + k, N)}, device_id_type=MESH
        )

    @pl.when(z > 0)
    def _():
        pl.semaphore_signal(barrier, inc=1, device_id={"ra": z - 1}, device_id_type=MESH)

    @pl.when(z < R - 1)
    def _():
        pl.semaphore_signal(barrier, inc=1, device_id={"ra": z + 1}, device_id_type=MESH)

    def split(block):
        return [
            block[:, c * Dc : (c + 1) * Dc].reshape(RG, SEQ_LEN, Dc).astype(jnp.bfloat16)
            for c in range(CG)
        ]

    def joined(q):
        parts = [
            xs[q, c * RG : (c + 1) * RG].astype(jnp.float32).reshape(rows, Dc)
            for c in range(CG)
        ]
        return jnp.concatenate(parts, axis=1) if CG > 1 else parts[0]

    def take(i, carry):
        at = pl.ds(pl.multiple_of(i * rows, rows), rows)
        for c, piece in enumerate(split(tokens_ref[at, :].astype(jnp.float32))):
            xs[i, c * RG : (c + 1) * RG] = piece
        return carry

    lax.fori_loop(0, n, take, 0)

    par[...] = jnp.zeros_like(par)
    for l in range(L):
        par[l, 0:1, 0:F] = gs_ref[l : l + 1, :]
        par[l, 1:2, 0:F] = vs_ref[l : l + 1, :]
        par[l, 2:3, 0:F] = gb_ref[l : l + 1, :]
        par[l, 3:4, 0:F] = vb_ref[l : l + 1, :]
        for k in range(taps):
            par[l, 4 + k : 5 + k, 0:F] = gc_ref[k, l : l + 1, :]
            par[l, 4 + taps + k : 5 + taps + k, 0:F] = vc_ref[k, l : l + 1, :]

    def cast_rows(dst, l, first, src, start, count, step):
        def move(b, carry):
            to = pl.ds(pl.multiple_of(first + b * step, step), step)
            at = pl.ds(pl.multiple_of(start + b * step, step), step)
            dst[l, to, :] = src[at, :].astype(jnp.bfloat16)
            return carry

        lax.fori_loop(0, count // step, move, 0)

    def fetch(l, k):
        if l < L:
            weight_copy(l, k).start()

    def cast_up(l):
        weight_copy(l, 0).wait()
        cast_rows(wc, l, 0, stage_g, 0, full, 64)
        cast_rows(wc, l, 2 * full, stage_g, full, rest, 32)
        fetch(l + 1, 0)
        weight_copy(l, 1).wait()
        cast_rows(wc, l, full, stage_v, 0, full, 64)
        cast_rows(wc, l, 2 * full + rest, stage_v, full, rest, 32)
        wc[l, 2 * F :, :] = jnp.zeros((wc.shape[1] - 2 * F, Dl), jnp.bfloat16)
        fetch(l + 1, 1)

    def cast_down(l):
        weight_copy(l, 2).wait()
        cast_rows(wd, l, 0, stage_d, 0, F, 32)
        wd[l, F:wide, :] = jnp.zeros((wide - F, Dl), jnp.bfloat16)
        fetch(l + 1, 2)

    pieces_up = full // 64
    lag = pieces_up // 4
    pieces_down = -(-(F // 32) // (pieces_up - lag))

    def cast_piece(l, c):
        @pl.when(c == 0)
        def _():
            weight_copy(l, 0).wait()
            weight_copy(l, 1).wait()
            cast_rows(wc, l, 2 * full, stage_g, full, rest, 32)
            cast_rows(wc, l, 2 * full + rest, stage_v, full, rest, 32)
            wc[l, 2 * F :, :] = jnp.zeros((wc.shape[1] - 2 * F, Dl), jnp.bfloat16)

        @pl.when(c == lag)
        def _():
            weight_copy(l, 2).wait()
            wd[l, F:wide, :] = jnp.zeros((wide - F, Dl), jnp.bfloat16)

        cast_rows(wc, l, c * 64, stage_g, c * 64, 64, 64)
        cast_rows(wc, l, full + c * 64, stage_v, c * 64, 64, 64)
        for k in range(pieces_down):

            b = (c - lag) * pieces_down + k

            @pl.when((b >= 0) & (b < F // 32))
            def _():
                cast_rows(wd, l, b * 32, stage_d, b * 32, 32, 32)

        @pl.when(c == pieces_up - 1)
        def _():
            for k in range(3):
                fetch(l + 1, k)

    cast_up(0)

    expected = N - 1 + jnp.where(z > 0, 1, 0) + jnp.where(z < R - 1, 1, 0)
    pl.semaphore_wait(barrier, expected)

    def when_item(g, fn):
        layer = lax.div(g, S)
        i = lax.rem(g, S)

        @pl.when((g >= 0) & (g < L * S) & (i < n))
        def _():
            fn(layer, i, layer * n + i)

    def part_copy(q, d, target):
        return pltpu.make_async_remote_copy(
            src_ref=pout.at[q, d],
            dst_ref=pin.at[q, d],
            send_sem=ps.at[q, d],
            recv_sem=pr.at[q, d],
            device_id={"ra": target},
            device_id_type=MESH,
        )

    def hid_copy(q, d, target):
        return pltpu.make_async_remote_copy(
            src_ref=hid.at[q, d],
            dst_ref=hid.at[q, d],
            send_sem=hs.at[q, d],
            recv_sem=hr.at[q, d],
            device_id={"ra": target},
            device_id_type=MESH,
        )

    row_in_seq = lax.rem(lax.broadcasted_iota(jnp.int32, (m, wide), 0), SEQ_LEN)
    lane = lax.broadcasted_iota(jnp.int32, (m, LANES), 1)

    def conv(values, l, first):
        total = values * par[l, first + taps - 1 : first + taps, :]
        for back in range(1, taps):
            moved = jnp.where(row_in_seq >= back, pltpu.roll(values, back, 0), 0.0)
            total = total + moved * par[l, first + taps - 1 - back : first + taps - back, :]
        return total

    def finish(l, q, d, main_g, main_v, tail):
        squares = jnp.sum(
            jnp.where((lane == sq_lane) | (lane == sq_lane + 1), tail, 0.0),
            axis=1,
            keepdims=True,
        )
        inverse = lax.rsqrt(squares / D + EPSILON)
        gate = jnp.concatenate([main_g, tail], axis=1)
        value = jnp.concatenate([main_v, pltpu.roll(tail, LANES - rest, 1)], axis=1)
        gate = gate * inverse * par[l, 0:1, :]
        value = value * inverse * par[l, 1:2, :]
        gate = par[l, 2:3, :] + conv(gate, l, 4)
        value = par[l, 3:4, :] + conv(value, l, 4 + taps)
        hid[q, d] = (gate / (1.0 + jnp.exp(-gate)) * value).astype(jnp.bfloat16)

    def chain(d, l, q):
        first = (z == 0) if d == 0 else (z == R - 1)
        last = (z == R - 1) if d == 0 else (z == 0)
        ahead = z + 1 if d == 0 else z - 1
        behind = z - 1 if d == 0 else z + 1

        def send(main_g, main_v, tail):
            squares = jnp.sum(
                jnp.where((lane == sq_lane) | (lane == sq_lane + 1), tail, 0.0),
                axis=1,
                keepdims=True,
            )
            high = squares.astype(jnp.bfloat16).astype(jnp.float32)
            tail = jnp.where(
                lane == sq_lane,
                high,
                jnp.where(lane == sq_lane + 1, squares - high, tail),
            )
            pout[q, d, :, 0:full] = main_g.astype(jnp.bfloat16)
            pout[q, d, :, full : 2 * full] = main_v.astype(jnp.bfloat16)
            pout[q, d, :, 2 * full : 2 * full + LANES] = tail.astype(jnp.bfloat16)
            part_copy(q, d, ahead).start()

        def pieces(ref):
            return (
                ref[q, d, :, 0:full].astype(jnp.float32),
                ref[q, d, :, full : 2 * full].astype(jnp.float32),
                ref[q, d, :, 2 * full : 2 * full + LANES].astype(jnp.float32),
            )

        @pl.when(first)
        def _():
            send(*pieces(own))

        @pl.when(jnp.logical_not(first))
        def _():
            part_copy(q, d, behind).wait_recv()
            summed = tuple(a + b for a, b in zip(pieces(own), pieces(pin)))

            @pl.when(last)
            def _():
                finish(l, q, d, *summed)
                hid_copy(q, d, behind).start()

            @pl.when(jnp.logical_not(last))
            def _():
                send(*summed)

    def spread_back(d, l, q):
        source = z + 1 if d == 0 else z - 1
        onward = z - 1 if d == 0 else z + 1
        last = (z == 0) if d == 0 else (z == R - 1)
        hid_copy(q, d, source).wait_recv()

        @pl.when(jnp.logical_not(last))
        def _():
            hid_copy(q, d, onward).start()

    def peer_copy(src, dst, send_sem, recv_sem, peer):
        return pltpu.make_async_remote_copy(
            src_ref=src,
            dst_ref=dst,
            send_sem=send_sem,
            recv_sem=recv_sem,
            device_id={"cb": peer},
            device_id_type=MESH,
        )

    def wait_group(ref, q, sem):
        view = ref.at[q, 0 : N - 1]
        pltpu.make_async_copy(view, view, sem).wait()

    def down_and_scatter(l, i, q):
        h = hid[q].reshape(rows, wide)
        product = jnp.dot(h, wd[l], preferred_element_type=jnp.float32)
        for c, piece in enumerate(split(product)):
            ro[q, c * RG : (c + 1) * RG] = piece
        for k in range(1, N):
            peer = lax.rem(me + k, N)
            peer_copy(
                ro.at[q, peer], ri.at[q, me], rs_s.at[q], rs_r.at[q], peer
            ).start()
        ri[q, me] = ro[q, me]

    def sum_and_gather(l, i, q):
        wait_group(ri, q, rs_r.at[q])
        total = ri[q, 0].astype(jnp.float32)
        for k in range(1, N):
            total = total + ri[q, k].astype(jnp.float32)
        scales = ds_ref[pl.ds(l, 1), :]
        mine = lax.div(me, RG)
        scale = scales[:, 0:Dc]
        for c in range(1, CG):
            scale = jnp.where(mine == c, scales[:, c * Dc : (c + 1) * Dc], scale)
        branch = total * scale
        fresh = RESIDUAL_KEEP * xs[q, me].astype(jnp.float32) + branch
        xs[q + n, me] = fresh.astype(jnp.bfloat16)
        for k in range(1, N):
            peer = lax.rem(me + k, N)
            peer_copy(
                xs.at[q + n, me], xs.at[q + n, me], ag_s.at[q], ag_r.at[q], peer
            ).start()

    def gathered(l, i, q):
        wait_group(xs, q + n, ag_r.at[q])

        @pl.when(l == L - 1)
        def _():
            block = joined(q + n)
            at = pl.ds(pl.multiple_of(i * rows, rows), rows)
            out_ref[at, :] = block.astype(jnp.bfloat16)

    def products(l, i, q):
        x = joined(q)
        squares = jnp.sum(x * x, axis=1, keepdims=True)
        normed = (x * gain_ref[pl.ds(l, 1), :]).astype(jnp.bfloat16)
        result = lax.dot_general(
            normed,
            wc[l],
            (((1,), (1,)), ((), ())),
            preferred_element_type=jnp.float32,
        )
        tail_lane = lax.broadcasted_iota(jnp.int32, (rows, LANES), 1)
        tail = jnp.where(tail_lane == sq_lane, squares, result[:, 2 * full :])
        for d in range(2):
            part = slice(d * m, (d + 1) * m)
            own[q, d, :, 0 : 2 * full] = result[part, 0 : 2 * full]
            own[q, d, :, 2 * full :] = tail[part]

    def slot(t, carry):
        when_item(t - FIRST - HOP * z, lambda l, i, q: chain(0, l, q))
        when_item(t - FIRST - HOP * (R - 1 - z), lambda l, i, q: chain(1, l, q))

        @pl.when(z < R - 1)
        def _():
            ago = at_last + BACK * (R - 1 - z)
            when_item(t - ago, lambda l, i, q: spread_back(0, l, q))

        @pl.when(z > 0)
        def _():
            when_item(t - at_last - BACK * z, lambda l, i, q: spread_back(1, l, q))

        when_item(t - at_down, down_and_scatter)
        when_item(t - at_sum, sum_and_gather)
        when_item(t - at_gather, gathered)
        when_item(t, products)
        pl.when(t == 1)(functools.partial(cast_down, 0))
        for l in range(1, L):
            c = t - l * S + pieces_up

            @pl.when((c >= 0) & (c < pieces_up))
            def _():
                cast_piece(l, c)

        return carry

    lax.fori_loop(0, (L - 1) * S + n + at_gather, slot, 0)

    def drain(q, carry):
        @pl.when(z < R - 1)
        def _():
            part_copy(q, 0, z + 1).wait_send()
            hid_copy(q, 1, z + 1).wait_send()

        @pl.when(z > 0)
        def _():
            part_copy(q, 1, z - 1).wait_send()
            hid_copy(q, 0, z - 1).wait_send()

        wait_group(ro, q, rs_s.at[q])
        wait_group(xs, q + n, ag_s.at[q])
        return carry

    lax.fori_loop(0, L * n, drain, 0)


def solution(mesh):
    R, N = mesh.shape["ra"], mesh.shape["cb"]

    def shards(*args):
        args = list(args)
        for k in (2, 4):
            args[k] = jnp.swapaxes(args[k], 1, 2)
        for k in (6, 7):
            args[k] = jnp.swapaxes(args[k], 0, 1)
        tokens, gw = args[0], args[2]
        T, Dl = tokens.shape
        L, F, _ = gw.shape
        m = 16
        if N * SEQ_LEN > 2 * m and Dl % (N * SEQ_LEN // (2 * m) * LANES):
            m = N * SEQ_LEN // 2
        rows = 2 * m
        parts = N * SEQ_LEN // rows
        n = T // rows
        full = F // LANES * LANES
        wide = full + LANES
        packed = 2 * full + LANES
        cfg = (R, N, L, n, m, Dl * R, F)
        Q = L * n
        bf16, f32 = jnp.bfloat16, jnp.float32
        dma = pltpu.SemaphoreType.DMA
        vmem = pl.BlockSpec(memory_space=pltpu.VMEM)
        hbm = pl.BlockSpec(memory_space=pl.ANY)
        in_specs = [hbm if k in (2, 4, 10) else vmem for k in range(12)]
        return pl.pallas_call(
            functools.partial(kernel, cfg),
            out_shape=jax.ShapeDtypeStruct((T, Dl), bf16),
            in_specs=in_specs,
            out_specs=vmem,
            scratch_shapes=[
                pltpu.VMEM((F, Dl), f32),
                pltpu.VMEM((F, Dl), f32),
                pltpu.VMEM((F, Dl), f32),
                pltpu.VMEM((L, packed, Dl), bf16),
                pltpu.VMEM((L, wide, Dl), bf16),
                pltpu.VMEM((L, 16, wide), f32),
                pltpu.VMEM((Q + n, N, SEQ_LEN, Dl // parts), bf16),
                pltpu.VMEM((Q, 2, m, packed), f32),
                pltpu.VMEM((Q, 2, m, packed), bf16),
                pltpu.VMEM((Q, 2, m, packed), bf16),
                pltpu.VMEM((Q, 2, m, wide), bf16),
                pltpu.VMEM((Q, N, SEQ_LEN, Dl // parts), bf16),
                pltpu.VMEM((Q, N, SEQ_LEN, Dl // parts), bf16),
                dma((3,)),
                dma((Q, 2)),
                dma((Q, 2)),
                dma((Q, 2)),
                dma((Q, 2)),
                dma((Q,)),
                dma((Q,)),
                dma((Q,)),
                dma((Q,)),
            ],
            compiler_params=pltpu.CompilerParams(
                collective_id=0,
                has_side_effects=True,
                vmem_limit_bytes=67043328,
            ),
        )(*args)

    placed = (
        P(None, "ra"),
        P(None, "ra"),
        P(None, "ra", "cb"),
        P(None, "cb"),
        P(None, "ra", "cb"),
        P(None, "cb"),
        P(None, None, "cb"),
        P(None, None, "cb"),
        P(None, "cb"),
        P(None, "cb"),
        P(None, "cb", "ra"),
        P(None, "ra"),
    )
    return jax.shard_map(
        shards, mesh=mesh, in_specs=placed, out_specs=P(None, "ra"), check_vma=False
    )
```

```python
import functools
import jax
import jax.numpy as jnp
from jax import lax
from jax.experimental import pallas as pl
from jax.experimental.pallas import tpu as pltpu
from jax.sharding import PartitionSpec as P

SEQ_LEN = 8
EPSILON = 1e-06
RESIDUAL_KEEP = 0.5
MESH = pl.DeviceIdType.MESH
LANES = 128
FIRST = 1
HOP = 2
BACK = 2
SUM_GAP = 2
GATHER_GAP = 2
DIRECT = 2
DIRECT_GAP = 3


def kernel(
    cfg,
    tokens_in,
    gain_in,
    gw_ref,
    gs_in,
    vw_ref,
    vs_in,
    gc_in,
    vc_in,
    gb_in,
    vb_in,
    dw_ref,
    ds_in,
    out_ref,
    tokens_ref,
    gain_ref,
    gs_ref,
    vs_ref,
    gc_ref,
    vc_ref,
    gb_ref,
    vb_ref,
    ds_ref,
    stage_g,
    stage_v,
    stage_d,
    wc,
    wd,
    par,
    xs,
    own,
    pin,
    pout,
    hid,
    ro,
    ri,
    w_sem,
    first_sem,
    in_sem,
    ps,
    pr,
    hs,
    hs_far,
    hr,
    rs_s,
    rs_r,
    ag_s,
    ag_r,
):
    R, N, L, n, m, D, F = cfg
    Dl = tokens_ref.shape[1]
    rows = 2 * m
    RG = rows // SEQ_LEN
    CG = N // RG
    Dc = Dl // CG
    taps = gc_ref.shape[0]
    full = F // LANES * LANES
    rest = F - full
    wide = full + LANES
    sq_lane = 2 * rest
    at_last = FIRST + (R - 1) * HOP
    at_down = at_last + (R - 1) * BACK
    at_sum = at_down + SUM_GAP
    at_gather = at_sum + GATHER_GAP
    S = max(n, at_gather)
    K = hs_far.shape[0]
    far_down = at_last + DIRECT_GAP
    far_sum = far_down + SUM_GAP
    far_gather = far_sum + GATHER_GAP
    outer = L * n - K
    z = lax.axis_index("ra")
    me = lax.axis_index("cb")

    def weight_copy(l, k):
        src, dst = ((gw_ref, stage_g), (vw_ref, stage_v), (dw_ref, stage_d))[k]
        return pltpu.make_async_copy(src.at[l], dst, w_sem.at[k])

    small = (
        (tokens_in, tokens_ref),
        (gain_in, gain_ref),
        (gs_in, gs_ref),
        (vs_in, vs_ref),
        (gc_in, gc_ref),
        (vc_in, vc_ref),
        (gb_in, gb_ref),
        (vb_in, vb_ref),
        (ds_in, ds_ref),
    )
    inputs = [
        pltpu.make_async_copy(src, dst, in_sem.at[k])
        for k, (src, dst) in enumerate(small)
    ]

    barrier = pltpu.get_barrier_semaphore()
    for k in range(1, N):
        pl.semaphore_signal(
            barrier, inc=1, device_id={"cb": lax.rem(me + k, N)}, device_id_type=MESH
        )

    @pl.when(z > 0)
    def _():
        pl.semaphore_signal(barrier, inc=1, device_id={"ra": z - 1}, device_id_type=MESH)

    @pl.when(z < R - 1)
    def _():
        pl.semaphore_signal(barrier, inc=1, device_id={"ra": z + 1}, device_id_type=MESH)

    C = first_sem.shape[1]
    step = full // C

    def first_copy(k, c):
        src, dst = ((gw_ref, stage_g), (vw_ref, stage_v))[k]
        at = pl.ds(c * step, step + (rest if c == C - 1 else 0))
        return pltpu.make_async_copy(
            src.at[0, at, :], dst.at[at, :], first_sem.at[k, c]
        )

    inputs[0].start()
    inputs[1].start()
    for c in range(C):
        first_copy(0, c).start()
        first_copy(1, c).start()
    for k in range(2, len(inputs)):
        inputs[k].start()
    weight_copy(0, 2).start()

    def split(block):
        return [
            block[:, c * Dc : (c + 1) * Dc].reshape(RG, SEQ_LEN, Dc).astype(jnp.bfloat16)
            for c in range(CG)
        ]

    def joined(q):
        parts = [
            xs[q, c * RG : (c + 1) * RG].astype(jnp.float32).reshape(rows, Dc)
            for c in range(CG)
        ]
        return jnp.concatenate(parts, axis=1) if CG > 1 else parts[0]

    def take(i):
        at = pl.ds(pl.multiple_of(i * rows, rows), rows)
        for c, piece in enumerate(split(tokens_ref[at, :].astype(jnp.float32))):
            xs[i, c * RG : (c + 1) * RG] = piece

    inputs[0].wait()
    take(0)

    def set_par():
        for k in range(2, len(inputs)):
            inputs[k].wait()
        par[...] = jnp.zeros_like(par)
        for l in range(L):
            par[l, 0:1, 0:F] = gs_ref[l : l + 1, :]
            par[l, 1:2, 0:F] = vs_ref[l : l + 1, :]
            par[l, 2:3, 0:F] = gb_ref[l : l + 1, :]
            par[l, 3:4, 0:F] = vb_ref[l : l + 1, :]
            for k in range(taps):
                par[l, 4 + k : 5 + k, 0:F] = gc_ref[k, l : l + 1, :]
                par[l, 4 + taps + k : 5 + taps + k, 0:F] = vc_ref[k, l : l + 1, :]

    def cast_rows(dst, l, first, src, start, count, step):
        def move(b, carry):
            to = pl.ds(pl.multiple_of(first + b * step, step), step)
            at = pl.ds(pl.multiple_of(start + b * step, step), step)
            dst[l, to, :] = src[at, :].astype(jnp.bfloat16)
            return carry

        lax.fori_loop(0, count // step, move, 0)

    def fetch(l, k):
        if l < L:
            weight_copy(l, k).start()

    def cast_rest(l):
        cast_rows(wc, l, 2 * full, stage_g, full, rest, 32)
        cast_rows(wc, l, 2 * full + rest, stage_v, full, rest, 32)
        wc[l, 2 * F :, :] = jnp.zeros((wc.shape[1] - 2 * F, Dl), jnp.bfloat16)

    up_rows = full // 8
    down_rows = 96

    def cast_up_piece(l, c):
        @pl.when(c == 0)
        def _():
            weight_copy(l, 0).wait()
            weight_copy(l, 1).wait()
            cast_rest(l)

        cast_rows(wc, l, c * up_rows, stage_g, c * up_rows, up_rows, 64)
        cast_rows(wc, l, full + c * up_rows, stage_v, c * up_rows, up_rows, 64)

        @pl.when(c == 7)
        def _():
            fetch(l + 1, 0)
            fetch(l + 1, 1)

    def cast_down_piece(l, c):
        @pl.when(c == 0)
        def _():
            weight_copy(l, 2).wait()
            wd[l, F:wide, :] = jnp.zeros((wide - F, Dl), jnp.bfloat16)

        cast_rows(wd, l, c * down_rows, stage_d, c * down_rows, down_rows, 32)

        @pl.when(c == F // down_rows - 1)
        def _():
            fetch(l + 1, 2)

    def normalised(l, q):
        x = joined(q)
        squares = jnp.sum(x * x, axis=1, keepdims=True)
        return squares, (x * gain_ref[pl.ds(l, 1), :]).astype(jnp.bfloat16)

    def times_up(normed, l, lo, hi):
        return lax.dot_general(
            normed,
            wc[l, lo:hi, :],
            (((1,), (1,)), ((), ())),
            preferred_element_type=jnp.float32,
        )

    def keep(q, lo, hi, result):
        for d in range(2):
            own[q, d, :, lo:hi] = result[d * m : (d + 1) * m]

    def keep_tail(q, result, squares):
        at = lax.broadcasted_iota(jnp.int32, (rows, LANES), 1)
        keep(q, 2 * full, 2 * full + LANES, jnp.where(at == sq_lane, squares, result))

    inputs[1].wait()
    squares, normed = normalised(0, 0)
    for c in range(C):
        first_copy(0, c).wait()
        cast_rows(wc, 0, c * step, stage_g, c * step, step, 64)
        keep(0, c * step, (c + 1) * step, times_up(normed, 0, c * step, (c + 1) * step))
        first_copy(1, c).wait()
        lo = full + c * step
        cast_rows(wc, 0, lo, stage_v, c * step, step, 64)
        keep(0, lo, lo + step, times_up(normed, 0, lo, lo + step))
    cast_rest(0)
    keep_tail(0, times_up(normed, 0, 2 * full, 2 * full + LANES), squares)

    set_par()
    for k in range(2):
        fetch(1, k)
    expected = N - 1 + jnp.where(z > 0, 1, 0) + jnp.where(z < R - 1, 1, 0)
    pl.semaphore_wait(barrier, expected)

    def when_item(g, fn, end=L * n):
        layer = lax.div(g, S)
        i = lax.rem(g, S)
        q = layer * n + i

        @pl.when((g >= 0) & (g < L * S) & (i < n) & (q < end))
        def _():
            fn(layer, i, q)

    def when_far(g, fn):
        i = g - (L - 1) * S

        @pl.when((i >= n - K) & (i < n))
        def _():
            fn(L - 1, i, (L - 1) * n + i)

    def part_copy(q, d, target):
        return pltpu.make_async_remote_copy(
            src_ref=pout.at[q, d],
            dst_ref=pin.at[q, d],
            send_sem=ps.at[q, d],
            recv_sem=pr.at[q, d],
            device_id={"ra": target},
            device_id_type=MESH,
        )

    def hid_copy(q, d, target):
        return pltpu.make_async_remote_copy(
            src_ref=hid.at[q, d],
            dst_ref=hid.at[q, d],
            send_sem=hs.at[q, d],
            recv_sem=hr.at[q, d],
            device_id={"ra": target},
            device_id_type=MESH,
        )

    def far_copy(q, d, k):
        return pltpu.make_async_remote_copy(
            src_ref=hid.at[q, d],
            dst_ref=hid.at[q, d],
            send_sem=hs_far.at[q - outer, d, k],
            recv_sem=hr.at[q, d],
            device_id={"ra": k if d == 0 else R - 1 - k},
            device_id_type=MESH,
        )

    row_in_seq = lax.rem(lax.broadcasted_iota(jnp.int32, (m, wide), 0), SEQ_LEN)
    lane = lax.broadcasted_iota(jnp.int32, (m, LANES), 1)

    def conv(values, l, first):
        total = values * par[l, first + taps - 1 : first + taps, :]
        for back in range(1, taps):
            moved = jnp.where(row_in_seq >= back, pltpu.roll(values, back, 0), 0.0)
            total = total + moved * par[l, first + taps - 1 - back : first + taps - back, :]
        return total

    def finish(l, q, d, main_g, main_v, tail):
        squares = jnp.sum(
            jnp.where((lane == sq_lane) | (lane == sq_lane + 1), tail, 0.0),
            axis=1,
            keepdims=True,
        )
        inverse = lax.rsqrt(squares / D + EPSILON)
        gate = jnp.concatenate([main_g, tail], axis=1)
        value = jnp.concatenate([main_v, pltpu.roll(tail, LANES - rest, 1)], axis=1)
        gate = gate * inverse * par[l, 0:1, :]
        value = value * inverse * par[l, 1:2, :]
        gate = par[l, 2:3, :] + conv(gate, l, 4)
        value = par[l, 3:4, :] + conv(value, l, 4 + taps)
        hid[q, d] = (gate / (1.0 + jnp.exp(-gate)) * value).astype(jnp.bfloat16)

    def chain(d, l, q):
        first = (z == 0) if d == 0 else (z == R - 1)
        last = (z == R - 1) if d == 0 else (z == 0)
        ahead = z + 1 if d == 0 else z - 1
        behind = z - 1 if d == 0 else z + 1

        def send(main_g, main_v, tail):
            squares = jnp.sum(
                jnp.where((lane == sq_lane) | (lane == sq_lane + 1), tail, 0.0),
                axis=1,
                keepdims=True,
            )
            high = squares.astype(jnp.bfloat16).astype(jnp.float32)
            tail = jnp.where(
                lane == sq_lane,
                high,
                jnp.where(lane == sq_lane + 1, squares - high, tail),
            )
            pout[q, d, :, 0:full] = main_g.astype(jnp.bfloat16)
            pout[q, d, :, full : 2 * full] = main_v.astype(jnp.bfloat16)
            pout[q, d, :, 2 * full : 2 * full + LANES] = tail.astype(jnp.bfloat16)
            part_copy(q, d, ahead).start()

        def pieces(ref):
            return (
                ref[q, d, :, 0:full].astype(jnp.float32),
                ref[q, d, :, full : 2 * full].astype(jnp.float32),
                ref[q, d, :, 2 * full : 2 * full + LANES].astype(jnp.float32),
            )

        @pl.when(first)
        def _():
            send(*pieces(own))

        @pl.when(jnp.logical_not(first))
        def _():
            part_copy(q, d, behind).wait_recv()
            summed = tuple(a + b for a, b in zip(pieces(own), pieces(pin)))

            @pl.when(last)
            def _():
                finish(l, q, d, *summed)

                @pl.when(q < outer)
                def _():
                    hid_copy(q, d, behind).start()

                @pl.when(q >= outer)
                def _():
                    for k in range(R - 1):
                        far_copy(q, d, k).start()

            @pl.when(jnp.logical_not(last))
            def _():
                send(*summed)

    def spread_back(d, l, q):
        source = z + 1 if d == 0 else z - 1
        onward = z - 1 if d == 0 else z + 1
        last = (z == 0) if d == 0 else (z == R - 1)
        hid_copy(q, d, source).wait_recv()

        @pl.when(jnp.logical_not(last))
        def _():
            hid_copy(q, d, onward).start()

    def peer_copy(src, dst, send_sem, recv_sem, peer):
        return pltpu.make_async_remote_copy(
            src_ref=src,
            dst_ref=dst,
            send_sem=send_sem,
            recv_sem=recv_sem,
            device_id={"cb": peer},
            device_id_type=MESH,
        )

    def wait_group(ref, q, sem):
        view = ref.at[q, 0 : N - 1]
        pltpu.make_async_copy(view, view, sem).wait()

    def down_and_scatter(l, i, q):
        h = hid[q].reshape(rows, wide)
        product = jnp.dot(h, wd[l], preferred_element_type=jnp.float32)
        for c, piece in enumerate(split(product)):
            ro[q, c * RG : (c + 1) * RG] = piece
        for k in range(1, N):
            peer = lax.rem(me + k, N)
            peer_copy(
                ro.at[q, peer], ri.at[q, me], rs_s.at[q], rs_r.at[q], peer
            ).start()
        ri[q, me] = ro[q, me]

    def sum_and_gather(l, i, q):
        wait_group(ri, q, rs_r.at[q])
        total = ri[q, 0].astype(jnp.float32)
        for k in range(1, N):
            total = total + ri[q, k].astype(jnp.float32)
        scales = ds_ref[pl.ds(l, 1), :]
        mine = lax.div(me, RG)
        scale = scales[:, 0:Dc]
        for c in range(1, CG):
            scale = jnp.where(mine == c, scales[:, c * Dc : (c + 1) * Dc], scale)
        branch = total * scale
        fresh = RESIDUAL_KEEP * xs[q, me].astype(jnp.float32) + branch
        xs[q + n, me] = fresh.astype(jnp.bfloat16)
        for k in range(1, N):
            peer = lax.rem(me + k, N)
            peer_copy(
                xs.at[q + n, me], xs.at[q + n, me], ag_s.at[q], ag_r.at[q], peer
            ).start()

    def gathered(l, i, q):
        wait_group(xs, q + n, ag_r.at[q])

        @pl.when(l == L - 1)
        def _():
            block = joined(q + n)
            at = pl.ds(pl.multiple_of(i * rows, rows), rows)
            out_ref[at, :] = block.astype(jnp.bfloat16)

    def products(l, i, q):
        squares, normed = normalised(l, q)
        result = times_up(normed, l, 0, 2 * full + LANES)
        keep(q, 0, 2 * full, result[:, 0 : 2 * full])
        keep_tail(q, result[:, 2 * full :], squares)

    def far_down_and_scatter(l, i, q):
        @pl.when(z < R - 1)
        def _():
            hid_copy(q, 0, z).wait_recv()

        @pl.when(z > 0)
        def _():
            hid_copy(q, 1, z).wait_recv()

        down_and_scatter(l, i, q)

    def slot(t, carry):

        @pl.when(z < R - 1)
        def _():
            ago = at_last + BACK * (R - 1 - z)
            when_item(t - ago, lambda l, i, q: spread_back(0, l, q), outer)

        @pl.when(z > 0)
        def _():
            ago = at_last + BACK * z
            when_item(t - ago, lambda l, i, q: spread_back(1, l, q), outer)

        when_item(t - at_down, down_and_scatter, outer)
        when_far(t - far_down, far_down_and_scatter)
        when_item(t - at_sum, sum_and_gather, outer)
        when_far(t - far_sum, sum_and_gather)
        when_item(t - FIRST - HOP * z, lambda l, i, q: chain(0, l, q))
        when_item(t - FIRST - HOP * (R - 1 - z), lambda l, i, q: chain(1, l, q))
        when_item(t - at_gather, gathered, outer)
        when_far(t - far_gather, gathered)
        pl.when(t < n)(lambda: take(t))
        when_item(t, products)

        pl.when((t >= 2) & (t < 2 + F // down_rows))(
            functools.partial(cast_down_piece, 0, t - 2)
        )
        for l in range(1, L):
            c = t - (l - 1) * S - 4
            pl.when((c >= 0) & (c < 8))(functools.partial(cast_up_piece, l, c))
            pl.when((c >= 10) & (c < 10 + F // down_rows))(
                functools.partial(cast_down_piece, l, c - 10)
            )

        return carry

    slots = max(n - K + at_gather, n + far_gather)
    lax.fori_loop(1, (L - 1) * S + slots, slot, 0)

    def drain(q, carry):
        @pl.when(z < R - 1)
        def _():
            part_copy(q, 0, z + 1).wait_send()

        @pl.when(z > 0)
        def _():
            part_copy(q, 1, z - 1).wait_send()

        @pl.when((z < R - 1) & (q < outer))
        def _():
            hid_copy(q, 1, z + 1).wait_send()

        @pl.when((z > 0) & (q < outer))
        def _():
            hid_copy(q, 0, z - 1).wait_send()

        for k in range(R - 1):

            @pl.when((z == R - 1) & (q >= outer))
            def _():
                far_copy(q, 0, k).wait_send()

            @pl.when((z == 0) & (q >= outer))
            def _():
                far_copy(q, 1, k).wait_send()

        wait_group(ro, q, rs_s.at[q])
        wait_group(xs, q + n, ag_s.at[q])
        return carry

    lax.fori_loop(0, L * n, drain, 0)


def solution(mesh):
    R, N = mesh.shape["ra"], mesh.shape["cb"]

    def shards(*args):
        args = list(args)
        for k in (2, 4):
            args[k] = jnp.swapaxes(args[k], 1, 2)
        for k in (6, 7):
            args[k] = jnp.swapaxes(args[k], 0, 1)
        tokens, gw = args[0], args[2]
        T, Dl = tokens.shape
        L, F, _ = gw.shape
        m = 16
        if N * SEQ_LEN > 2 * m and Dl % (N * SEQ_LEN // (2 * m) * LANES):
            m = N * SEQ_LEN // 2
        rows = 2 * m
        parts = N * SEQ_LEN // rows
        n = T // rows
        full = F // LANES * LANES
        wide = full + LANES
        packed = 2 * full + LANES
        cfg = (R, N, L, n, m, Dl * R, F)
        Q = L * n
        bf16, f32 = jnp.bfloat16, jnp.float32
        dma = pltpu.SemaphoreType.DMA
        hbm = pl.BlockSpec(memory_space=pl.ANY)
        in_specs = [hbm] * len(args)
        staged = [
            pltpu.VMEM(a.shape, a.dtype)
            for k, a in enumerate(args)
            if k not in (2, 4, 10)
        ]
        held = pl.pallas_call(
            functools.partial(kernel, cfg),
            out_shape=pltpu.VMEM((T, Dl), bf16),
            in_specs=in_specs,
            out_specs=pl.BlockSpec(memory_space=pltpu.VMEM),
            scratch_shapes=staged
            + [
                pltpu.VMEM((F, Dl), f32),
                pltpu.VMEM((F, Dl), f32),
                pltpu.VMEM((F, Dl), f32),
                pltpu.VMEM((L, packed, Dl), bf16),
                pltpu.VMEM((L, wide, Dl), bf16),
                pltpu.VMEM((L, 16, wide), f32),
                pltpu.VMEM((Q + n, N, SEQ_LEN, Dl // parts), bf16),
                pltpu.VMEM((Q, 2, m, packed), f32),
                pltpu.VMEM((Q, 2, m, packed), bf16),
                pltpu.VMEM((Q, 2, m, packed), bf16),
                pltpu.VMEM((Q, 2, m, wide), bf16),
                pltpu.VMEM((Q, N, SEQ_LEN, Dl // parts), bf16),
                pltpu.VMEM((Q, N, SEQ_LEN, Dl // parts), bf16),
                dma((3,)),
                dma((2, 4)),
                dma((len(staged),)),
                dma((Q, 2)),
                dma((Q, 2)),
                dma((Q, 2)),
                dma((min(DIRECT, n), 2, R - 1)),
                dma((Q, 2)),
                dma((Q,)),
                dma((Q,)),
                dma((Q,)),
                dma((Q,)),
            ],
            compiler_params=pltpu.CompilerParams(
                collective_id=0,
                has_side_effects=True,
                vmem_limit_bytes=60 * 2**20,
            ),
        )(*args)
        return held

    placed = (
        P(None, "ra"),
        P(None, "ra"),
        P(None, "ra", "cb"),
        P(None, "cb"),
        P(None, "ra", "cb"),
        P(None, "cb"),
        P(None, None, "cb"),
        P(None, None, "cb"),
        P(None, "cb"),
        P(None, "cb"),
        P(None, "cb", "ra"),
        P(None, "ra"),
    )
    return jax.shard_map(
        shards, mesh=mesh, in_specs=placed, out_specs=P(None, "ra"), check_vma=False
    )
```

```python
import functools
import jax
import jax.numpy as jnp
from jax import lax
from jax.experimental import pallas as pl
from jax.experimental.pallas import tpu as pltpu
from jax.sharding import PartitionSpec as P

SEQ_LEN = 8
EPSILON = 1e-06
RESIDUAL_KEEP = 0.5
MESH = pl.DeviceIdType.MESH
LANES = 128
FIRST = 1
HOP = 2
BACK = 2
SUM_GAP = 2
GATHER_GAP = 2
DIRECT = 3
DIRECT_GAP = 3


def kernel(
    cfg,
    tokens_in,
    gain_in,
    gw_ref,
    gs_in,
    vw_ref,
    vs_in,
    gc_in,
    vc_in,
    gb_in,
    vb_in,
    dw_ref,
    ds_in,
    out_ref,
    tokens_ref,
    gain_ref,
    gs_ref,
    vs_ref,
    gc_ref,
    vc_ref,
    gb_ref,
    vb_ref,
    ds_ref,
    stage_g,
    stage_v,
    stage_d,
    wc,
    wd,
    par,
    xs,
    own,
    pin,
    pout,
    hid,
    ro,
    ri,
    w_sem,
    first_sem,
    in_sem,
    ps,
    pr,
    hs,
    hs_far,
    hr,
    rs_s,
    rs_r,
    ag_s,
    ag_r,
):
    R, N, L, n, m, D, F = cfg
    Dl = tokens_ref.shape[1]
    rows = 2 * m
    RG = rows // SEQ_LEN
    CG = N // RG
    Dc = Dl // CG
    taps = gc_ref.shape[0]
    full = F // LANES * LANES
    rest = F - full
    wide = full + LANES
    sq_lane = 2 * rest
    at_last = FIRST + (R - 1) * HOP
    at_down = at_last + (R - 1) * BACK
    at_sum = at_down + SUM_GAP
    at_gather = at_sum + GATHER_GAP
    S = max(n, at_gather)
    K = hs_far.shape[0]
    far_down = at_last + DIRECT_GAP
    far_sum = far_down + SUM_GAP
    far_gather = far_sum + GATHER_GAP
    outer = L * n - K
    z = lax.axis_index("ra")
    me = lax.axis_index("cb")

    def weight_copy(l, k):
        src, dst = ((gw_ref, stage_g), (vw_ref, stage_v), (dw_ref, stage_d))[k]
        return pltpu.make_async_copy(src.at[l], dst, w_sem.at[k])

    small = (
        (tokens_in, tokens_ref),
        (gain_in, gain_ref),
        (gs_in, gs_ref),
        (vs_in, vs_ref),
        (gc_in, gc_ref),
        (vc_in, vc_ref),
        (gb_in, gb_ref),
        (vb_in, vb_ref),
        (ds_in, ds_ref),
    )
    inputs = [
        pltpu.make_async_copy(src, dst, in_sem.at[k])
        for k, (src, dst) in enumerate(small)
    ]

    barrier = pltpu.get_barrier_semaphore()
    for k in range(1, N):
        pl.semaphore_signal(
            barrier, inc=1, device_id={"cb": lax.rem(me + k, N)}, device_id_type=MESH
        )

    @pl.when(z > 0)
    def _():
        pl.semaphore_signal(barrier, inc=1, device_id={"ra": z - 1}, device_id_type=MESH)

    @pl.when(z < R - 1)
    def _():
        pl.semaphore_signal(barrier, inc=1, device_id={"ra": z + 1}, device_id_type=MESH)

    C = first_sem.shape[1]
    step = full // C

    def first_copy(k, c):
        src, dst = ((gw_ref, stage_g), (vw_ref, stage_v))[k]
        at = pl.ds(c * step, step + (rest if c == C - 1 else 0))
        return pltpu.make_async_copy(
            src.at[0, at, :], dst.at[at, :], first_sem.at[k, c]
        )

    inputs[0].start()
    inputs[1].start()
    for c in range(C):
        first_copy(0, c).start()
        first_copy(1, c).start()
    for k in range(2, len(inputs)):
        inputs[k].start()
    weight_copy(0, 2).start()

    def split(block):
        return [
            block[:, c * Dc : (c + 1) * Dc].reshape(RG, SEQ_LEN, Dc).astype(jnp.bfloat16)
            for c in range(CG)
        ]

    def joined(q):
        parts = [
            xs[q, c * RG : (c + 1) * RG].astype(jnp.float32).reshape(rows, Dc)
            for c in range(CG)
        ]
        return jnp.concatenate(parts, axis=1) if CG > 1 else parts[0]

    def take(i):
        at = pl.ds(pl.multiple_of(i * rows, rows), rows)
        for c, piece in enumerate(split(tokens_ref[at, :].astype(jnp.float32))):
            xs[i, c * RG : (c + 1) * RG] = piece

    inputs[0].wait()
    take(0)

    def set_par():
        for k in range(2, len(inputs)):
            inputs[k].wait()
        par[...] = jnp.zeros_like(par)
        for l in range(L):
            par[l, 0:1, 0:F] = gs_ref[l : l + 1, :]
            par[l, 1:2, 0:F] = vs_ref[l : l + 1, :]
            par[l, 2:3, 0:F] = gb_ref[l : l + 1, :]
            par[l, 3:4, 0:F] = vb_ref[l : l + 1, :]
            for k in range(taps):
                par[l, 4 + k : 5 + k, 0:F] = gc_ref[k, l : l + 1, :]
                par[l, 4 + taps + k : 5 + taps + k, 0:F] = vc_ref[k, l : l + 1, :]

    def cast_rows(dst, l, first, src, start, count, step):
        def move(b, carry):
            to = pl.ds(pl.multiple_of(first + b * step, step), step)
            at = pl.ds(pl.multiple_of(start + b * step, step), step)
            dst[l, to, :] = src[at, :].astype(jnp.bfloat16)
            return carry

        lax.fori_loop(0, count // step, move, 0)

    def fetch(l, k):
        if l < L:
            weight_copy(l, k).start()

    def cast_rest(l):
        cast_rows(wc, l, 2 * full, stage_g, full, rest, 32)
        cast_rows(wc, l, 2 * full + rest, stage_v, full, rest, 32)
        wc[l, 2 * F :, :] = jnp.zeros((wc.shape[1] - 2 * F, Dl), jnp.bfloat16)

    up_rows = full // 8
    down_rows = 96

    def cast_up_piece(l, c):
        @pl.when(c == 0)
        def _():
            weight_copy(l, 0).wait()
            weight_copy(l, 1).wait()
            cast_rest(l)

        cast_rows(wc, l, c * up_rows, stage_g, c * up_rows, up_rows, 64)
        cast_rows(wc, l, full + c * up_rows, stage_v, c * up_rows, up_rows, 64)

        @pl.when(c == 7)
        def _():
            fetch(l + 1, 0)
            fetch(l + 1, 1)

    def cast_down_piece(l, c):
        @pl.when(c == 0)
        def _():
            weight_copy(l, 2).wait()
            wd[l, F:wide, :] = jnp.zeros((wide - F, Dl), jnp.bfloat16)

        cast_rows(wd, l, c * down_rows, stage_d, c * down_rows, down_rows, 32)

        @pl.when(c == F // down_rows - 1)
        def _():
            fetch(l + 1, 2)

    def normalised(l, q):
        x = joined(q)
        squares = jnp.sum(x * x, axis=1, keepdims=True)
        return squares, (x * gain_ref[pl.ds(l, 1), :]).astype(jnp.bfloat16)

    def times_up(normed, l, lo, hi):
        return lax.dot_general(
            normed,
            wc[l, lo:hi, :],
            (((1,), (1,)), ((), ())),
            preferred_element_type=jnp.float32,
        )

    def keep(q, lo, hi, result):
        for d in range(2):
            own[q, d, :, lo:hi] = result[d * m : (d + 1) * m]

    def keep_tail(q, result, squares):
        at = lax.broadcasted_iota(jnp.int32, (rows, LANES), 1)
        keep(q, 2 * full, 2 * full + LANES, jnp.where(at == sq_lane, squares, result))

    inputs[1].wait()
    squares, normed = normalised(0, 0)
    for c in range(C):
        first_copy(0, c).wait()
        cast_rows(wc, 0, c * step, stage_g, c * step, step, 64)
        keep(0, c * step, (c + 1) * step, times_up(normed, 0, c * step, (c + 1) * step))
        first_copy(1, c).wait()
        lo = full + c * step
        cast_rows(wc, 0, lo, stage_v, c * step, step, 64)
        keep(0, lo, lo + step, times_up(normed, 0, lo, lo + step))
    cast_rest(0)
    keep_tail(0, times_up(normed, 0, 2 * full, 2 * full + LANES), squares)

    set_par()
    for k in range(2):
        fetch(1, k)
    expected = N - 1 + jnp.where(z > 0, 1, 0) + jnp.where(z < R - 1, 1, 0)
    pl.semaphore_wait(barrier, expected)

    def when_item(g, fn, end=L * n):
        layer = lax.div(g, S)
        i = lax.rem(g, S)
        q = layer * n + i

        @pl.when((g >= 0) & (g < L * S) & (i < n) & (q < end))
        def _():
            fn(layer, i, q)

    def when_far(g, fn):
        i = g - (L - 1) * S

        @pl.when((i >= n - K) & (i < n))
        def _():
            fn(L - 1, i, (L - 1) * n + i)

    def part_copy(q, d, target):
        return pltpu.make_async_remote_copy(
            src_ref=pout.at[q, d],
            dst_ref=pin.at[q, d],
            send_sem=ps.at[q, d],
            recv_sem=pr.at[q, d],
            device_id={"ra": target},
            device_id_type=MESH,
        )

    def hid_copy(q, d, target):
        return pltpu.make_async_remote_copy(
            src_ref=hid.at[q, d],
            dst_ref=hid.at[q, d],
            send_sem=hs.at[q, d],
            recv_sem=hr.at[q, d],
            device_id={"ra": target},
            device_id_type=MESH,
        )

    def far_copy(q, d, k):
        return pltpu.make_async_remote_copy(
            src_ref=hid.at[q, d],
            dst_ref=hid.at[q, d],
            send_sem=hs_far.at[q - outer, d, k],
            recv_sem=hr.at[q, d],
            device_id={"ra": k if d == 0 else R - 1 - k},
            device_id_type=MESH,
        )

    row_in_seq = lax.rem(lax.broadcasted_iota(jnp.int32, (m, wide), 0), SEQ_LEN)
    lane = lax.broadcasted_iota(jnp.int32, (m, LANES), 1)
    tail_lane = lax.broadcasted_iota(jnp.int32, (SEQ_LEN, LANES), 1)
    G = m // SEQ_LEN
    tiles = full // LANES

    def conv(values, l, first):
        total = values * par[l, first + taps - 1 : first + taps, :]
        for back in range(1, taps):
            moved = jnp.where(row_in_seq >= back, pltpu.roll(values, back, 0), 0.0)
            total = total + moved * par[l, first + taps - 1 - back : first + taps - back, :]
        return total

    def finish(l, q, d, main_g, main_v, tail):
        squares = jnp.sum(
            jnp.where((lane == sq_lane) | (lane == sq_lane + 1), tail, 0.0),
            axis=1,
            keepdims=True,
        )
        inverse = lax.rsqrt(squares / D + EPSILON)
        gate = jnp.concatenate([main_g, tail], axis=1)
        value = jnp.concatenate([main_v, pltpu.roll(tail, LANES - rest, 1)], axis=1)
        gate = gate * inverse * par[l, 0:1, :]
        value = value * inverse * par[l, 1:2, :]
        gate = par[l, 2:3, :] + conv(gate, l, 4)
        value = par[l, 3:4, :] + conv(value, l, 4 + taps)
        hidden = gate / (1.0 + jnp.exp(-gate)) * value
        packed = jnp.zeros((SEQ_LEN, LANES), jnp.float32)
        for g in range(G):
            piece = hidden[g * SEQ_LEN : (g + 1) * SEQ_LEN, :]
            for c in range(tiles):
                part = piece[:, c * LANES : (c + 1) * LANES]
                hid[q, d, g * tiles + c] = part.astype(jnp.bfloat16)
            piece = jnp.where(tail_lane < rest, piece[:, full:wide], 0.0)
            packed = packed + (pltpu.roll(piece, g * rest, 1) if g else piece)
        hid[q, d, G * tiles] = packed.astype(jnp.bfloat16)

    def chain(d, l, q):
        first = (z == 0) if d == 0 else (z == R - 1)
        last = (z == R - 1) if d == 0 else (z == 0)
        ahead = z + 1 if d == 0 else z - 1
        behind = z - 1 if d == 0 else z + 1

        def send(main_g, main_v, tail):
            squares = jnp.sum(
                jnp.where((lane == sq_lane) | (lane == sq_lane + 1), tail, 0.0),
                axis=1,
                keepdims=True,
            )
            high = squares.astype(jnp.bfloat16).astype(jnp.float32)
            tail = jnp.where(
                lane == sq_lane,
                high,
                jnp.where(lane == sq_lane + 1, squares - high, tail),
            )
            pout[q, d, :, 0:full] = main_g.astype(jnp.bfloat16)
            pout[q, d, :, full : 2 * full] = main_v.astype(jnp.bfloat16)
            pout[q, d, :, 2 * full : 2 * full + LANES] = tail.astype(jnp.bfloat16)
            part_copy(q, d, ahead).start()

        def pieces(ref):
            return (
                ref[q, d, :, 0:full].astype(jnp.float32),
                ref[q, d, :, full : 2 * full].astype(jnp.float32),
                ref[q, d, :, 2 * full : 2 * full + LANES].astype(jnp.float32),
            )

        @pl.when(first)
        def _():
            send(*pieces(own))

        @pl.when(jnp.logical_not(first))
        def _():
            part_copy(q, d, behind).wait_recv()
            summed = tuple(a + b for a, b in zip(pieces(own), pieces(pin)))

            @pl.when(last)
            def _():
                finish(l, q, d, *summed)

                @pl.when(q < outer)
                def _():
                    hid_copy(q, d, behind).start()

                @pl.when(q >= outer)
                def _():
                    for k in range(R - 1):
                        far_copy(q, d, k).start()

            @pl.when(jnp.logical_not(last))
            def _():
                send(*summed)

    def spread_back(d, l, q):
        source = z + 1 if d == 0 else z - 1
        onward = z - 1 if d == 0 else z + 1
        last = (z == 0) if d == 0 else (z == R - 1)
        hid_copy(q, d, source).wait_recv()

        @pl.when(jnp.logical_not(last))
        def _():
            hid_copy(q, d, onward).start()

    def peer_copy(src, dst, send_sem, recv_sem, peer):
        return pltpu.make_async_remote_copy(
            src_ref=src,
            dst_ref=dst,
            send_sem=send_sem,
            recv_sem=recv_sem,
            device_id={"cb": peer},
            device_id_type=MESH,
        )

    def wait_group(ref, q, sem):
        view = ref.at[q, 0 : N - 1]
        pltpu.make_async_copy(view, view, sem).wait()

    def down_and_scatter(l, i, q):
        lines = []
        for d in range(2):
            packed = hid[q, d, G * tiles].astype(jnp.float32)
            for g in range(G):
                line = [hid[q, d, g * tiles + c].astype(jnp.float32) for c in range(tiles)]
                piece = pltpu.roll(packed, LANES - g * rest, 1) if g else packed
                line.append(jnp.where(tail_lane < rest, piece, 0.0))
                lines.append(jnp.concatenate(line, axis=1))
        h = jnp.concatenate(lines, axis=0).astype(jnp.bfloat16)
        product = jnp.dot(h, wd[l], preferred_element_type=jnp.float32)
        for c, piece in enumerate(split(product)):
            ro[q, c * RG : (c + 1) * RG] = piece
        for k in range(1, N):
            peer = lax.rem(me + k, N)
            peer_copy(
                ro.at[q, peer], ri.at[q, me], rs_s.at[q], rs_r.at[q], peer
            ).start()
        ri[q, me] = ro[q, me]

    def sum_and_gather(l, i, q):
        wait_group(ri, q, rs_r.at[q])
        total = ri[q, 0].astype(jnp.float32)
        for k in range(1, N):
            total = total + ri[q, k].astype(jnp.float32)
        scales = ds_ref[pl.ds(l, 1), :]
        mine = lax.div(me, RG)
        scale = scales[:, 0:Dc]
        for c in range(1, CG):
            scale = jnp.where(mine == c, scales[:, c * Dc : (c + 1) * Dc], scale)
        branch = total * scale
        fresh = RESIDUAL_KEEP * xs[q, me].astype(jnp.float32) + branch
        xs[q + n, me] = fresh.astype(jnp.bfloat16)
        for k in range(1, N):
            peer = lax.rem(me + k, N)
            peer_copy(
                xs.at[q + n, me], xs.at[q + n, me], ag_s.at[q], ag_r.at[q], peer
            ).start()

    def gathered(l, i, q):
        wait_group(xs, q + n, ag_r.at[q])

        @pl.when(l == L - 1)
        def _():
            block = joined(q + n)
            at = pl.ds(pl.multiple_of(i * rows, rows), rows)
            out_ref[at, :] = block.astype(jnp.bfloat16)

    def products(l, i, q):
        squares, normed = normalised(l, q)
        result = times_up(normed, l, 0, 2 * full + LANES)
        keep(q, 0, 2 * full, result[:, 0 : 2 * full])
        keep_tail(q, result[:, 2 * full :], squares)

    def far_down_and_scatter(l, i, q):
        @pl.when(z < R - 1)
        def _():
            hid_copy(q, 0, z).wait_recv()

        @pl.when(z > 0)
        def _():
            hid_copy(q, 1, z).wait_recv()

        down_and_scatter(l, i, q)

    def slot(t, carry):

        @pl.when(z < R - 1)
        def _():
            ago = at_last + BACK * (R - 1 - z)
            when_item(t - ago, lambda l, i, q: spread_back(0, l, q), outer)

        @pl.when(z > 0)
        def _():
            ago = at_last + BACK * z
            when_item(t - ago, lambda l, i, q: spread_back(1, l, q), outer)

        when_item(t - at_down, down_and_scatter, outer)
        when_far(t - far_down, far_down_and_scatter)
        when_item(t - at_sum, sum_and_gather, outer)
        when_far(t - far_sum, sum_and_gather)
        when_item(t - FIRST - HOP * z, lambda l, i, q: chain(0, l, q))
        when_item(t - FIRST - HOP * (R - 1 - z), lambda l, i, q: chain(1, l, q))
        when_item(t - at_gather, gathered, outer)
        when_far(t - far_gather, gathered)
        pl.when(t < n)(lambda: take(t))
        when_item(t, products)

        pl.when((t >= 2) & (t < 2 + F // down_rows))(
            functools.partial(cast_down_piece, 0, t - 2)
        )
        for l in range(1, L):
            c = t - (l - 1) * S - 4
            pl.when((c >= 0) & (c < 8))(functools.partial(cast_up_piece, l, c))
            pl.when((c >= 10) & (c < 10 + F // down_rows))(
                functools.partial(cast_down_piece, l, c - 10)
            )

        return carry

    slots = max(n - K + at_gather, n + far_gather)
    lax.fori_loop(1, (L - 1) * S + slots, slot, 0)

    def drain(q, carry):
        @pl.when(z < R - 1)
        def _():
            part_copy(q, 0, z + 1).wait_send()

        @pl.when(z > 0)
        def _():
            part_copy(q, 1, z - 1).wait_send()

        @pl.when((z < R - 1) & (q < outer))
        def _():
            hid_copy(q, 1, z + 1).wait_send()

        @pl.when((z > 0) & (q < outer))
        def _():
            hid_copy(q, 0, z - 1).wait_send()

        for k in range(R - 1):

            @pl.when((z == R - 1) & (q >= outer))
            def _():
                far_copy(q, 0, k).wait_send()

            @pl.when((z == 0) & (q >= outer))
            def _():
                far_copy(q, 1, k).wait_send()

        wait_group(ro, q, rs_s.at[q])
        wait_group(xs, q + n, ag_s.at[q])
        return carry

    lax.fori_loop(0, L * n, drain, 0)


def solution(mesh):
    R, N = mesh.shape["ra"], mesh.shape["cb"]

    def shards(*args):
        args = list(args)
        for k in (2, 4):
            args[k] = jnp.swapaxes(args[k], 1, 2)
        for k in (6, 7):
            args[k] = jnp.swapaxes(args[k], 0, 1)
        tokens, gw = args[0], args[2]
        T, Dl = tokens.shape
        L, F, _ = gw.shape
        m = 16
        if N * SEQ_LEN > 2 * m and Dl % (N * SEQ_LEN // (2 * m) * LANES):
            m = N * SEQ_LEN // 2
        rows = 2 * m
        parts = N * SEQ_LEN // rows
        n = T // rows
        full = F // LANES * LANES
        wide = full + LANES
        packed = 2 * full + LANES
        cfg = (R, N, L, n, m, Dl * R, F)
        Q = L * n
        bf16, f32 = jnp.bfloat16, jnp.float32
        dma = pltpu.SemaphoreType.DMA
        hbm = pl.BlockSpec(memory_space=pl.ANY)
        in_specs = [hbm] * len(args)
        staged = [
            pltpu.VMEM(a.shape, a.dtype)
            for k, a in enumerate(args)
            if k not in (2, 4, 10)
        ]
        held = pl.pallas_call(
            functools.partial(kernel, cfg),
            out_shape=pltpu.VMEM((T, Dl), bf16),
            in_specs=in_specs,
            out_specs=pl.BlockSpec(memory_space=pltpu.VMEM),
            scratch_shapes=staged
            + [
                pltpu.VMEM((F, Dl), f32),
                pltpu.VMEM((F, Dl), f32),
                pltpu.VMEM((F, Dl), f32),
                pltpu.VMEM((L, packed, Dl), bf16),
                pltpu.VMEM((L, wide, Dl), bf16),
                pltpu.VMEM((L, 16, wide), f32),
                pltpu.VMEM((Q + n, N, SEQ_LEN, Dl // parts), bf16),
                pltpu.VMEM((Q, 2, m, packed), f32),
                pltpu.VMEM((Q, 2, m, packed), bf16),
                pltpu.VMEM((Q, 2, m, packed), bf16),
                pltpu.VMEM((Q, 2, m // SEQ_LEN * (full // LANES) + 1, SEQ_LEN, LANES), bf16),
                pltpu.VMEM((Q, N, SEQ_LEN, Dl // parts), bf16),
                pltpu.VMEM((Q, N, SEQ_LEN, Dl // parts), bf16),
                dma((3,)),
                dma((2, 4)),
                dma((len(staged),)),
                dma((Q, 2)),
                dma((Q, 2)),
                dma((Q, 2)),
                dma((min(DIRECT, n), 2, R - 1)),
                dma((Q, 2)),
                dma((Q,)),
                dma((Q,)),
                dma((Q,)),
                dma((Q,)),
            ],
            compiler_params=pltpu.CompilerParams(
                collective_id=0,
                has_side_effects=True,
                vmem_limit_bytes=60 * 2**20,
            ),
        )(*args)
        return held

    placed = (
        P(None, "ra"),
        P(None, "ra"),
        P(None, "ra", "cb"),
        P(None, "cb"),
        P(None, "ra", "cb"),
        P(None, "cb"),
        P(None, None, "cb"),
        P(None, None, "cb"),
        P(None, "cb"),
        P(None, "cb"),
        P(None, "cb", "ra"),
        P(None, "ra"),
    )
    return jax.shard_map(
        shards, mesh=mesh, in_specs=placed, out_specs=P(None, "ra"), check_vma=False
    )
```

```python
import functools
import jax
import jax.numpy as jnp
from jax import lax
from jax.experimental import pallas as pl
from jax.experimental.pallas import tpu as pltpu
from jax.sharding import PartitionSpec as P

SEQ_LEN = 8
EPSILON = 1e-06
RESIDUAL_KEEP = 0.5
MESH = pl.DeviceIdType.MESH
LANES = 128
FIRST = 1
HOP = 2
BACK = 2
SUM_GAP = 2
GATHER_GAP = 2
DIRECT = 3
DIRECT_GAP = 3


def kernel(
    cfg,
    tokens_in,
    gain_in,
    gw_ref,
    gs_in,
    vw_ref,
    vs_in,
    gc_in,
    vc_in,
    gb_in,
    vb_in,
    dw_ref,
    ds_in,
    out_ref,
    tokens_ref,
    gain_ref,
    gs_ref,
    vs_ref,
    gc_ref,
    vc_ref,
    gb_ref,
    vb_ref,
    ds_ref,
    stage_g,
    stage_v,
    stage_d,
    wc,
    wd,
    par,
    xs,
    own,
    pin,
    pout,
    hid,
    ro,
    ri,
    w_sem,
    first_sem,
    in_sem,
    ps,
    pr,
    hs,
    hs_far,
    hr,
    rs_s,
    rs_r,
    ag_s,
    ag_r,
):
    R, N, L, n, m, D, F = cfg
    Dl = tokens_ref.shape[1]
    rows = 2 * m
    RG = rows // SEQ_LEN
    CG = N // RG
    Dc = Dl // CG
    taps = gc_ref.shape[0]
    full = F // LANES * LANES
    rest = F - full
    wide = full + LANES
    sq_lane = 2 * rest
    at_last = FIRST + (R - 1) * HOP
    at_down = at_last + (R - 1) * BACK
    at_sum = at_down + SUM_GAP
    at_gather = at_sum + GATHER_GAP
    S = max(n, at_gather)
    K = hs_far.shape[0]
    far_down = at_last + DIRECT_GAP
    far_sum = far_down + SUM_GAP
    far_gather = far_sum + GATHER_GAP
    outer = L * n - K
    z = lax.axis_index("ra")
    me = lax.axis_index("cb")

    def weight_copy(l, k):
        src, dst = ((gw_ref, stage_g), (vw_ref, stage_v), (dw_ref, stage_d))[k]
        return pltpu.make_async_copy(src.at[l], dst, w_sem.at[k])

    small = (
        (tokens_in, tokens_ref),
        (gain_in, gain_ref),
        (gs_in, gs_ref),
        (vs_in, vs_ref),
        (gc_in, gc_ref),
        (vc_in, vc_ref),
        (gb_in, gb_ref),
        (vb_in, vb_ref),
        (ds_in, ds_ref),
    )
    inputs = [
        pltpu.make_async_copy(src, dst, in_sem.at[k])
        for k, (src, dst) in enumerate(small)
    ]

    barrier = pltpu.get_barrier_semaphore()
    @pl.when(z > 0)
    def _():
        pl.semaphore_signal(barrier, inc=1, device_id={"ra": z - 1}, device_id_type=MESH)

    @pl.when(z < R - 1)
    def _():
        pl.semaphore_signal(barrier, inc=1, device_id={"ra": z + 1}, device_id_type=MESH)

    for k in range(1, N):
        pl.semaphore_signal(
            barrier, inc=1, device_id={"cb": lax.rem(me + k, N)}, device_id_type=MESH
        )

    C = first_sem.shape[1]
    step = full // C

    def first_copy(k, c):
        src, dst = ((gw_ref, stage_g), (vw_ref, stage_v))[k]
        at = pl.ds(c * step, step + (rest if c == C - 1 else 0))
        return pltpu.make_async_copy(
            src.at[0, at, :], dst.at[at, :], first_sem.at[k, c]
        )

    inputs[0].start()
    inputs[1].start()
    for c in range(C):
        first_copy(0, c).start()
        first_copy(1, c).start()
    for k in range(2, len(inputs)):
        inputs[k].start()
    weight_copy(0, 2).start()

    def split(block):
        return [
            block[:, c * Dc : (c + 1) * Dc].reshape(RG, SEQ_LEN, Dc).astype(jnp.bfloat16)
            for c in range(CG)
        ]

    def joined(q):
        parts = [
            xs[q, c * RG : (c + 1) * RG].astype(jnp.float32).reshape(rows, Dc)
            for c in range(CG)
        ]
        return jnp.concatenate(parts, axis=1) if CG > 1 else parts[0]

    def take(i):
        at = pl.ds(pl.multiple_of(i * rows, rows), rows)
        for c, piece in enumerate(split(tokens_ref[at, :].astype(jnp.float32))):
            xs[i, c * RG : (c + 1) * RG] = piece

    inputs[0].wait()
    take(0)

    def set_par():
        for k in range(2, len(inputs)):
            inputs[k].wait()
        par[...] = jnp.zeros_like(par)
        for l in range(L):
            par[l, 0:1, 0:F] = gs_ref[l : l + 1, :]
            par[l, 1:2, 0:F] = vs_ref[l : l + 1, :]
            par[l, 2:3, 0:F] = gb_ref[l : l + 1, :]
            par[l, 3:4, 0:F] = vb_ref[l : l + 1, :]
            for k in range(taps):
                par[l, 4 + k : 5 + k, 0:F] = gc_ref[k, l : l + 1, :]
                par[l, 4 + taps + k : 5 + taps + k, 0:F] = vc_ref[k, l : l + 1, :]

    def cast_rows(dst, l, first, src, start, count, step):
        def move(b, carry):
            to = pl.ds(pl.multiple_of(first + b * step, step), step)
            at = pl.ds(pl.multiple_of(start + b * step, step), step)
            dst[l, to, :] = src[at, :].astype(jnp.bfloat16)
            return carry

        lax.fori_loop(0, count // step, move, 0)

    def fetch(l, k):
        if l < L:
            weight_copy(l, k).start()

    def cast_rest(l):
        cast_rows(wc, l, 2 * full, stage_g, full, rest, 32)
        cast_rows(wc, l, 2 * full + rest, stage_v, full, rest, 32)
        wc[l, 2 * F :, :] = jnp.zeros((wc.shape[1] - 2 * F, Dl), jnp.bfloat16)

    up_rows = full // 8
    down_rows = 96

    def cast_up_piece(l, c):
        @pl.when(c == 0)
        def _():
            weight_copy(l, 0).wait()
            weight_copy(l, 1).wait()
            cast_rest(l)

        cast_rows(wc, l, c * up_rows, stage_g, c * up_rows, up_rows, 64)
        cast_rows(wc, l, full + c * up_rows, stage_v, c * up_rows, up_rows, 64)

        @pl.when(c == 7)
        def _():
            fetch(l + 1, 0)
            fetch(l + 1, 1)

    def cast_down_piece(l, c):
        @pl.when(c == 0)
        def _():
            weight_copy(l, 2).wait()
            wd[l, F:wide, :] = jnp.zeros((wide - F, Dl), jnp.bfloat16)

        cast_rows(wd, l, c * down_rows, stage_d, c * down_rows, down_rows, 32)

        @pl.when(c == F // down_rows - 1)
        def _():
            fetch(l + 1, 2)

    def normalised(l, q):
        x = joined(q)
        squares = jnp.sum(x * x, axis=1, keepdims=True)
        return squares, (x * gain_ref[pl.ds(l, 1), :]).astype(jnp.bfloat16)

    def times_up(normed, l, lo, hi):
        return lax.dot_general(
            normed,
            wc[l, lo:hi, :],
            (((1,), (1,)), ((), ())),
            preferred_element_type=jnp.float32,
        )

    def keep(q, lo, hi, result):
        for d in range(2):
            own[q, d, :, lo:hi] = result[d * m : (d + 1) * m]

    def keep_tail(q, result, squares):
        at = lax.broadcasted_iota(jnp.int32, (rows, LANES), 1)
        keep(q, 2 * full, 2 * full + LANES, jnp.where(at == sq_lane, squares, result))

    inputs[1].wait()
    squares, normed = normalised(0, 0)
    for c in range(C):
        first_copy(0, c).wait()
        cast_rows(wc, 0, c * step, stage_g, c * step, step, 64)
        keep(0, c * step, (c + 1) * step, times_up(normed, 0, c * step, (c + 1) * step))
        first_copy(1, c).wait()
        lo = full + c * step
        cast_rows(wc, 0, lo, stage_v, c * step, step, 64)
        keep(0, lo, lo + step, times_up(normed, 0, lo, lo + step))
    cast_rest(0)
    keep_tail(0, times_up(normed, 0, 2 * full, 2 * full + LANES), squares)

    expected = N - 1 + jnp.where(z > 0, 1, 0) + jnp.where(z < R - 1, 1, 0)
    pl.semaphore_wait(barrier, expected)

    def when_item(g, fn, end=L * n):
        layer = lax.div(g, S)
        i = lax.rem(g, S)
        q = layer * n + i

        @pl.when((g >= 0) & (g < L * S) & (i < n) & (q < end))
        def _():
            fn(layer, i, q)

    def when_far(g, fn):
        i = g - (L - 1) * S

        @pl.when((i >= n - K) & (i < n))
        def _():
            fn(L - 1, i, (L - 1) * n + i)

    def part_copy(q, d, target):
        return pltpu.make_async_remote_copy(
            src_ref=pout.at[q, d],
            dst_ref=pin.at[q, d],
            send_sem=ps.at[q, d],
            recv_sem=pr.at[q, d],
            device_id={"ra": target},
            device_id_type=MESH,
        )

    def hid_copy(q, d, target):
        return pltpu.make_async_remote_copy(
            src_ref=hid.at[q, d],
            dst_ref=hid.at[q, d],
            send_sem=hs.at[q, d],
            recv_sem=hr.at[q, d],
            device_id={"ra": target},
            device_id_type=MESH,
        )

    def far_copy(q, d, k):
        return pltpu.make_async_remote_copy(
            src_ref=hid.at[q, d],
            dst_ref=hid.at[q, d],
            send_sem=hs_far.at[q - outer, d, k],
            recv_sem=hr.at[q, d],
            device_id={"ra": k if d == 0 else R - 1 - k},
            device_id_type=MESH,
        )

    row_in_seq = lax.rem(lax.broadcasted_iota(jnp.int32, (m, wide), 0), SEQ_LEN)
    lane = lax.broadcasted_iota(jnp.int32, (m, LANES), 1)
    tail_lane = lax.broadcasted_iota(jnp.int32, (SEQ_LEN, LANES), 1)
    G = m // SEQ_LEN
    tiles = full // LANES

    def conv(values, l, first):
        total = values * par[l, first + taps - 1 : first + taps, :]
        for back in range(1, taps):
            moved = jnp.where(row_in_seq >= back, pltpu.roll(values, back, 0), 0.0)
            total = total + moved * par[l, first + taps - 1 - back : first + taps - back, :]
        return total

    def finish(l, q, d, main_g, main_v, tail):
        squares = jnp.sum(
            jnp.where((lane == sq_lane) | (lane == sq_lane + 1), tail, 0.0),
            axis=1,
            keepdims=True,
        )
        inverse = lax.rsqrt(squares / D + EPSILON)
        gate = jnp.concatenate([main_g, tail], axis=1)
        value = jnp.concatenate([main_v, pltpu.roll(tail, LANES - rest, 1)], axis=1)
        gate = gate * inverse * par[l, 0:1, :]
        value = value * inverse * par[l, 1:2, :]
        gate = par[l, 2:3, :] + conv(gate, l, 4)
        value = par[l, 3:4, :] + conv(value, l, 4 + taps)
        hidden = gate / (1.0 + jnp.exp(-gate)) * value
        packed = jnp.zeros((SEQ_LEN, LANES), jnp.float32)
        for g in range(G):
            piece = hidden[g * SEQ_LEN : (g + 1) * SEQ_LEN, :]
            for c in range(tiles):
                part = piece[:, c * LANES : (c + 1) * LANES]
                hid[q, d, g * tiles + c] = part.astype(jnp.bfloat16)
            piece = jnp.where(tail_lane < rest, piece[:, full:wide], 0.0)
            packed = packed + (pltpu.roll(piece, g * rest, 1) if g else piece)
        hid[q, d, G * tiles] = packed.astype(jnp.bfloat16)

    def chain(d, l, q):
        first = (z == 0) if d == 0 else (z == R - 1)
        last = (z == R - 1) if d == 0 else (z == 0)
        ahead = z + 1 if d == 0 else z - 1
        behind = z - 1 if d == 0 else z + 1

        def send(main_g, main_v, tail):
            squares = jnp.sum(
                jnp.where((lane == sq_lane) | (lane == sq_lane + 1), tail, 0.0),
                axis=1,
                keepdims=True,
            )
            high = squares.astype(jnp.bfloat16).astype(jnp.float32)
            tail = jnp.where(
                lane == sq_lane,
                high,
                jnp.where(lane == sq_lane + 1, squares - high, tail),
            )
            pout[q, d, :, 0:full] = main_g.astype(jnp.bfloat16)
            pout[q, d, :, full : 2 * full] = main_v.astype(jnp.bfloat16)
            pout[q, d, :, 2 * full : 2 * full + LANES] = tail.astype(jnp.bfloat16)
            part_copy(q, d, ahead).start()

        def pieces(ref):
            return (
                ref[q, d, :, 0:full].astype(jnp.float32),
                ref[q, d, :, full : 2 * full].astype(jnp.float32),
                ref[q, d, :, 2 * full : 2 * full + LANES].astype(jnp.float32),
            )

        @pl.when(first)
        def _():
            send(*pieces(own))

        @pl.when(jnp.logical_not(first))
        def _():
            part_copy(q, d, behind).wait_recv()
            summed = tuple(a + b for a, b in zip(pieces(own), pieces(pin)))

            @pl.when(last)
            def _():
                finish(l, q, d, *summed)

                @pl.when(q < outer)
                def _():
                    hid_copy(q, d, behind).start()

                @pl.when(q >= outer)
                def _():
                    for k in range(R - 1):
                        far_copy(q, d, k).start()

            @pl.when(jnp.logical_not(last))
            def _():
                send(*summed)

    def spread_back(d, l, q):
        source = z + 1 if d == 0 else z - 1
        onward = z - 1 if d == 0 else z + 1
        last = (z == 0) if d == 0 else (z == R - 1)
        hid_copy(q, d, source).wait_recv()

        @pl.when(jnp.logical_not(last))
        def _():
            hid_copy(q, d, onward).start()

    def peer_copy(src, dst, send_sem, recv_sem, peer):
        return pltpu.make_async_remote_copy(
            src_ref=src,
            dst_ref=dst,
            send_sem=send_sem,
            recv_sem=recv_sem,
            device_id={"cb": peer},
            device_id_type=MESH,
        )

    def wait_group(ref, q, sem):
        view = ref.at[q, 0 : N - 1]
        pltpu.make_async_copy(view, view, sem).wait()

    def down_and_scatter(l, i, q):
        lines = []
        for d in range(2):
            packed = hid[q, d, G * tiles].astype(jnp.float32)
            for g in range(G):
                line = [hid[q, d, g * tiles + c].astype(jnp.float32) for c in range(tiles)]
                piece = pltpu.roll(packed, LANES - g * rest, 1) if g else packed
                line.append(jnp.where(tail_lane < rest, piece, 0.0))
                lines.append(jnp.concatenate(line, axis=1))
        h = jnp.concatenate(lines, axis=0).astype(jnp.bfloat16)
        product = jnp.dot(h, wd[l], preferred_element_type=jnp.float32)
        for c, piece in enumerate(split(product)):
            ro[q, c * RG : (c + 1) * RG] = piece
        for k in range(1, N):
            peer = lax.rem(me + k, N)
            peer_copy(
                ro.at[q, peer], ri.at[q, me], rs_s.at[q], rs_r.at[q], peer
            ).start()
        ri[q, me] = ro[q, me]

    def sum_and_gather(l, i, q):
        wait_group(ri, q, rs_r.at[q])
        total = ri[q, 0].astype(jnp.float32)
        for k in range(1, N):
            total = total + ri[q, k].astype(jnp.float32)
        scales = ds_ref[pl.ds(l, 1), :]
        mine = lax.div(me, RG)
        scale = scales[:, 0:Dc]
        for c in range(1, CG):
            scale = jnp.where(mine == c, scales[:, c * Dc : (c + 1) * Dc], scale)
        branch = total * scale
        fresh = RESIDUAL_KEEP * xs[q, me].astype(jnp.float32) + branch
        xs[q + n, me] = fresh.astype(jnp.bfloat16)
        for k in range(1, N):
            peer = lax.rem(me + k, N)
            peer_copy(
                xs.at[q + n, me], xs.at[q + n, me], ag_s.at[q], ag_r.at[q], peer
            ).start()

    def gathered(l, i, q):
        wait_group(xs, q + n, ag_r.at[q])

        @pl.when(l == L - 1)
        def _():
            block = joined(q + n)
            at = pl.ds(pl.multiple_of(i * rows, rows), rows)
            out_ref[at, :] = block.astype(jnp.bfloat16)

    def products(l, i, q):
        squares, normed = normalised(l, q)
        result = times_up(normed, l, 0, 2 * full + LANES)
        keep(q, 0, 2 * full, result[:, 0 : 2 * full])
        keep_tail(q, result[:, 2 * full :], squares)

    def far_down_and_scatter(l, i, q):
        @pl.when(z < R - 1)
        def _():
            hid_copy(q, 0, z).wait_recv()

        @pl.when(z > 0)
        def _():
            hid_copy(q, 1, z).wait_recv()

        down_and_scatter(l, i, q)

    def slot(t, carry):

        @pl.when(z < R - 1)
        def _():
            ago = at_last + BACK * (R - 1 - z)
            when_item(t - ago, lambda l, i, q: spread_back(0, l, q), outer)

        @pl.when(z > 0)
        def _():
            ago = at_last + BACK * z
            when_item(t - ago, lambda l, i, q: spread_back(1, l, q), outer)

        when_item(t - at_down, down_and_scatter, outer)
        when_far(t - far_down, far_down_and_scatter)
        when_item(t - at_sum, sum_and_gather, outer)
        when_far(t - far_sum, sum_and_gather)
        when_item(t - FIRST - HOP * z, lambda l, i, q: chain(0, l, q))
        when_item(t - FIRST - HOP * (R - 1 - z), lambda l, i, q: chain(1, l, q))
        when_item(t - at_gather, gathered, outer)
        when_far(t - far_gather, gathered)
        @pl.when(t == 1)
        def _():
            set_par()
            for k in range(2):
                fetch(1, k)

        pl.when(t < n)(lambda: take(t))
        when_item(t, products)

        pl.when((t >= 2) & (t < 2 + F // down_rows))(
            functools.partial(cast_down_piece, 0, t - 2)
        )
        for l in range(1, L):
            c = t - (l - 1) * S - 4
            pl.when((c >= 0) & (c < 8))(functools.partial(cast_up_piece, l, c))
            pl.when((c >= 10) & (c < 10 + F // down_rows))(
                functools.partial(cast_down_piece, l, c - 10)
            )

        return carry

    slots = max(n - K + at_gather, n + far_gather)
    lax.fori_loop(1, (L - 1) * S + slots, slot, 0)

    def drain(q, carry):
        @pl.when(z < R - 1)
        def _():
            part_copy(q, 0, z + 1).wait_send()

        @pl.when(z > 0)
        def _():
            part_copy(q, 1, z - 1).wait_send()

        @pl.when((z < R - 1) & (q < outer))
        def _():
            hid_copy(q, 1, z + 1).wait_send()

        @pl.when((z > 0) & (q < outer))
        def _():
            hid_copy(q, 0, z - 1).wait_send()

        for k in range(R - 1):

            @pl.when((z == R - 1) & (q >= outer))
            def _():
                far_copy(q, 0, k).wait_send()

            @pl.when((z == 0) & (q >= outer))
            def _():
                far_copy(q, 1, k).wait_send()

        wait_group(ro, q, rs_s.at[q])
        wait_group(xs, q + n, ag_s.at[q])
        return carry

    lax.fori_loop(0, L * n, drain, 0)


def solution(mesh):
    R, N = mesh.shape["ra"], mesh.shape["cb"]

    def shards(*args):
        args = list(args)
        for k in (2, 4):
            args[k] = jnp.swapaxes(args[k], 1, 2)
        for k in (6, 7):
            args[k] = jnp.swapaxes(args[k], 0, 1)
        tokens, gw = args[0], args[2]
        T, Dl = tokens.shape
        L, F, _ = gw.shape
        m = 16
        if N * SEQ_LEN > 2 * m and Dl % (N * SEQ_LEN // (2 * m) * LANES):
            m = N * SEQ_LEN // 2
        rows = 2 * m
        parts = N * SEQ_LEN // rows
        n = T // rows
        full = F // LANES * LANES
        wide = full + LANES
        packed = 2 * full + LANES
        cfg = (R, N, L, n, m, Dl * R, F)
        Q = L * n
        bf16, f32 = jnp.bfloat16, jnp.float32
        dma = pltpu.SemaphoreType.DMA
        hbm = pl.BlockSpec(memory_space=pl.ANY)
        in_specs = [hbm] * len(args)
        staged = [
            pltpu.VMEM(a.shape, a.dtype)
            for k, a in enumerate(args)
            if k not in (2, 4, 10)
        ]
        held = pl.pallas_call(
            functools.partial(kernel, cfg),
            out_shape=pltpu.VMEM((T, Dl), bf16),
            in_specs=in_specs,
            out_specs=pl.BlockSpec(memory_space=pltpu.VMEM),
            scratch_shapes=staged
            + [
                pltpu.VMEM((F, Dl), f32),
                pltpu.VMEM((F, Dl), f32),
                pltpu.VMEM((F, Dl), f32),
                pltpu.VMEM((L, packed, Dl), bf16),
                pltpu.VMEM((L, wide, Dl), bf16),
                pltpu.VMEM((L, 16, wide), f32),
                pltpu.VMEM((Q + n, N, SEQ_LEN, Dl // parts), bf16),
                pltpu.VMEM((Q, 2, m, packed), f32),
                pltpu.VMEM((Q, 2, m, packed), bf16),
                pltpu.VMEM((Q, 2, m, packed), bf16),
                pltpu.VMEM((Q, 2, m // SEQ_LEN * (full // LANES) + 1, SEQ_LEN, LANES), bf16),
                pltpu.VMEM((Q, N, SEQ_LEN, Dl // parts), bf16),
                pltpu.VMEM((Q, N, SEQ_LEN, Dl // parts), bf16),
                dma((3,)),
                dma((2, 4)),
                dma((len(staged),)),
                dma((Q, 2)),
                dma((Q, 2)),
                dma((Q, 2)),
                dma((min(DIRECT, n), 2, R - 1)),
                dma((Q, 2)),
                dma((Q,)),
                dma((Q,)),
                dma((Q,)),
                dma((Q,)),
            ],
            compiler_params=pltpu.CompilerParams(
                collective_id=0,
                has_side_effects=True,
                vmem_limit_bytes=60 * 2**20,
            ),
        )(*args)
        return held

    placed = (
        P(None, "ra"),
        P(None, "ra"),
        P(None, "ra", "cb"),
        P(None, "cb"),
        P(None, "ra", "cb"),
        P(None, "cb"),
        P(None, None, "cb"),
        P(None, None, "cb"),
        P(None, "cb"),
        P(None, "cb"),
        P(None, "cb", "ra"),
        P(None, "ra"),
    )
    return jax.shard_map(
        shards, mesh=mesh, in_specs=placed, out_specs=P(None, "ra"), check_vma=False
    )
```
